32 devices in a mesh: ep: 8 (over z, y), tp: 4 (over x, core).
Axes of the slice: x: 2, y: 2, z: 4, core: 2. Of those that a mesh axis runs over, the one named last changes fastest.
Arguments:
- queries: bfloat16 [1536, 2048], P('ep', 'tp'), may hold values from -5 to 5
- keys: bfloat16 [1536, 512], P('ep', 'tp'), may hold values from -5 to 5
- values: bfloat16 [1536, 512], P('ep', 'tp'), may hold values from -6 to 6
- query_gain: float32 [128], replicated, may hold values from 0.6 to 6
- key_gain: float32 [128], replicated, may hold values from 0.6 to 6
- out_weight: bfloat16 [2048, 2048], P('tp'), may hold values from -0.125 to 0.125
- mixer_gain: float32 [2048], replicated, may hold values from 0.1 to 1.9
- expert_in: bfloat16 [4096, 2048], P(('ep', 'tp')), may hold values from -6 to 6
- routes: int32 [4096, 2], P(('ep', 'tp')), may hold values from 0 to 7, all different within a row; in each aligned block of 128 rows (0 to 127, 128 to 255, ...) at most 48 rows name the same one
- route_weights: float32 [4096, 2], P(('ep', 'tp')), may hold values from 0.2 to 1
- expert_gain: float32 [2048], replicated, may hold values from 0.5 to 4
- gate_w: bfloat16 [8, 2048, 2048], P('ep', None, 'tp'), may hold values from -0.125 to 0.125
- up_w: bfloat16 [8, 2048, 2048], P('ep', None, 'tp'), may hold values from -0.125 to 0.125
- down_w: bfloat16 [8, 2048, 2048], P('ep', 'tp'), may hold values from -0.125 to 0.125
- ffn_out_gain: float32 [2048], replicated, may hold values from 0.1 to 1.9
Outputs:
- mixer_out: bfloat16 [1536, 2048], P(('ep', 'tp'))
- expert_out: bfloat16 [4096, 2048], P(('ep', 'tp'))
The draws below stay inside these ranges and needn't reach their ends.
Inputs may be any that keep to these rules, and one draw needn't show every extreme that they name: `routes`: each row names 2 different experts. Among the rows of one device no expert is named by more than 48 rows, and in every draw some expert is named by exactly 48 rows of some device.
All inputs are finite; a program needn't handle non-finite values.
Results may differ from the reference program's by a relative error of at most 0.015.
The reference program's roundings to bfloat16 on the way count: a program that leaves them out, or rounds other values in their place, can miss the bound.
Values may be sent and summed in bfloat16 or wider, within the bound.
A program may use at most 128 MiB of HBM per device.

```python
import math
import jax
import jax.numpy as jnp
import numpy as np
from jax import lax

D = 2048
HEADS = 16
KV_HEADS = 4
HEAD = 128
QW = 2048
KVW = 512
GRID_W = 64
LEN = 1536
FF = 2048
TOPK = 2
TB_DEV = 128
EXPERTS = 8
CAP = 48
TOKB = 4096
N_EP = 8
N_TP = 4


def plant_pairs(key):
    base_key = jax.random.fold_in(key, 7)
    key_part = jnp.clip(jax.random.normal(jax.random.fold_in(base_key, 1), (LEN, KVW), jnp.float32), -5.0, 5.0)
    query_part = jnp.clip(jax.random.normal(jax.random.fold_in(base_key, 2), (LEN, QW), jnp.float32), -5.0, 5.0)
    return (query_part, key_part)


def draw_queries(key, part):
    return plant_pairs(key)[0].astype(jnp.bfloat16)


def draw_keys(key, part):
    return plant_pairs(key)[1].astype(jnp.bfloat16)


def pair_gain(key, salt):
    base_key = jax.random.fold_in(key, salt)
    return jax.random.uniform(base_key, (HEAD,), jnp.float32, 0.6, 1.4)


def draw_query_gain(key, part):
    return pair_gain(key, 11)


def draw_key_gain(key, part):
    return pair_gain(key, 12)


def steps_of(key, shape, shards, least, top_value):
    def one(dim, blocks):
        heights = jax.random.uniform(jax.random.fold_in(jax.random.fold_in(key, 6), dim), (blocks,), jnp.float32, least / len(shards), top_value / len(shards))
        return jnp.repeat(jnp.exp(heights), shape[dim] // blocks).reshape((-1,) + (1,) * (len(shape) - dim - 1))

    level = one(*shards[0])
    for cut in shards[1:]:
        level = level * one(*cut)
    return level


def routed_block(stream_key, own, number, rows, number_of, top, most, slope):
    order = jax.random.permutation(stream_key, number_of)
    heavy_load, ordinary = shares(number_of, rows * top, most, slope, True), shares(number_of, rows * top, most, slope, False)
    places = jnp.arange(number_of)

    def named(tallies, turn):
        used = int((tallies > 0).sum())
        fixed = max(1, used // 4)
        shifted = fixed + (places - fixed + turn * (used - fixed)) % max(1, number_of - fixed)
        return jnp.zeros((number_of,), jnp.int32).at[order[jnp.where(places < fixed, places, shifted)]].set(jnp.asarray(tallies, jnp.int32))

    tallies = jnp.where(number % 4 == 0, named(heavy_load, number // 4), named(ordinary, number - number // 4 - 1))
    mixed = jax.random.permutation(jax.random.fold_in(own, 3), number_of)
    source_of, receiver = mixed[0:number_of // 2 * 2:2], mixed[1:number_of // 2 * 2:2]
    slack = jnp.minimum(tallies[source_of] - 1, most - tallies[receiver]) // 2
    slack = jnp.where((source_of == order[0]) | (receiver == order[0]) | (tallies[receiver] == 0), 0, jnp.maximum(slack, 0))
    shifted = jax.random.randint(jax.random.fold_in(own, 4), (number_of // 2,), 0, 1 << 20) % (slack + 1)
    tallies = tallies.at[source_of].add(-shifted).at[receiver].add(shifted)
    labels = jnp.searchsorted(jnp.cumsum(tallies), jnp.arange(rows * top), side="right").astype(jnp.int32)
    table = labels.reshape(top, rows).T
    table = table[jax.random.permutation(jax.random.fold_in(own, 1), rows)]
    turn = jax.random.randint(jax.random.fold_in(own, 2), (rows, 1), 0, top)
    return jnp.take_along_axis(table, (jnp.arange(top)[None, :] + turn) % top, axis=1)


def shares(number_of, total, most, lean, full):
    loads = [(1 << 20) // math.isqrt(standing ** lean) + 1 for standing in range(1, number_of + 1)]
    largest = most if full else min(most, max(-(-total // number_of), total * loads[0] // sum(loads)))
    least = 1 if total - largest >= number_of - 1 else 0
    given, spare = [largest] + [least] * (number_of - 1), total - largest - least * (number_of - 1)
    while spare > 0:
        movable = [i for i in range(1, number_of) if given[i] < largest] or [i for i in range(1, number_of) if given[i] < most]
        mass, left = sum([loads[i] for i in movable]), spare
        for i in movable:
            more = min(most - given[i], max(1, left * loads[i] // mass), spare)
            given[i] = given[i] + more
            spare = spare - more
    return np.array(given)


def scatter_about(key, shape, scale, reach, cuts=(), kind=jnp.bfloat16):
    entries = scale * jax.random.normal(key, shape, jnp.float32)
    if cuts:
        entries = entries * steps_of(key, shape, cuts, -0.22, 0.18)
    return jnp.clip(entries, -reach, reach).astype(kind)


def setup_inputs(seed: int = 0) -> dict:
    seeds = jax.random.split(jax.random.key(seed), 16)
    queries = draw_queries(jax.random.fold_in(seeds[15], 71), 0)
    keys = draw_keys(jax.random.fold_in(seeds[15], 71), 0)
    values = scatter_about(seeds[2], (LEN, KVW), 1.0, 6.0, ((0, 8), (1, 4)))
    query_gain = draw_query_gain(jax.random.fold_in(seeds[15], 71), 0)
    key_gain = draw_key_gain(jax.random.fold_in(seeds[15], 71), 0)
    out_weight = scatter_about(seeds[5], (QW, D), QW ** -0.5, 0.125, ((0, 4),))
    mixer_gain = jnp.clip(1.0 + 0.18 * jax.random.normal(seeds[6], (D,), jnp.float32), 0.1, 1.9)
    expert_in = scatter_about(seeds[7], (TOKB, D), 1.0, 6.0, ((0, 32),))
    routes_keys = jax.random.split(jax.random.fold_in(seeds[8], 1), TOKB // TB_DEV)
    routes_turns = jax.random.permutation(jax.random.fold_in(seeds[8], 3), TOKB // TB_DEV)
    routes = jax.vmap(lambda own, number: routed_block(jax.random.fold_in(seeds[8], 2), own, number, TB_DEV, EXPERTS, TOPK, CAP, 1))(routes_keys, routes_turns).reshape((TOKB, TOPK))
    route_weights = jnp.clip(0.2 + 0.8 * jax.random.uniform(seeds[9], (TOKB, TOPK), jnp.float32) ** steps_of(seeds[9], (TOKB, TOPK), ((0, 32),), -0.2, 0.2), 0.2, 1.0)
    expert_gain = jnp.clip(jnp.exp(jax.random.uniform(seeds[10], (D,), jnp.float32, math.log(0.5), math.log(4.0))), 0.5, 4.0)
    gate_w = scatter_about(seeds[11], (EXPERTS, D, FF), D ** -0.5, 0.125, ((0, 8), (2, 4)))
    up_w = scatter_about(seeds[12], (EXPERTS, D, FF), D ** -0.5, 0.125, ((0, 8), (2, 4)))
    down_w = scatter_about(seeds[13], (EXPERTS, FF, D), FF ** -0.5, 0.125, ((0, 8), (1, 4)))
    ffn_out_gain = jnp.clip(1.0 + 0.18 * jax.random.normal(seeds[14], (D,), jnp.float32), 0.1, 1.9)
    return {"queries": queries, "keys": keys, "values": values, "query_gain": query_gain, "key_gain": key_gain, "out_weight": out_weight, "mixer_gain": mixer_gain, "expert_in": expert_in, "routes": routes, "route_weights": route_weights, "expert_gain": expert_gain, "gate_w": gate_w, "up_w": up_w, "down_w": down_w, "ffn_out_gain": ffn_out_gain}


norm_eps = 1e-06
rope_base = 10000.0
clamp_limit = 7.0
sigmoid_slope = 1.702

def rms_scale(values_in, gain):
    return values_in * lax.rsqrt(lax.optimization_barrier(jnp.mean(values_in * values_in, axis=-1, keepdims=True)) + norm_eps) * gain

def turn_pair(halfpart, cosine, sine):
    first_part, second_part = jnp.split(halfpart, 2, axis=-1)
    return jnp.concatenate([first_part * cosine - second_part * sine, second_part * cosine + first_part * sine], axis=-1)

def grid_rotate(field, position):
    half_width = field.shape[-1] // 2
    inverse = rope_base ** (-jnp.arange(0, half_width, 2, dtype=jnp.float32) / half_width)
    grid_row = (position // GRID_W).astype(jnp.float32)
    grid_col = (position % GRID_W).astype(jnp.float32)
    row_angle = (grid_row[:, None] * inverse[None, :])[:, None, :]
    col_angle = (grid_col[:, None] * inverse[None, :])[:, None, :]
    return jnp.concatenate([turn_pair(field[..., :half_width], jnp.cos(row_angle), jnp.sin(row_angle)), turn_pair(field[..., half_width:], jnp.cos(col_angle), jnp.sin(col_angle))], axis=-1)

def clamped_unit(gate_pre, up_pre):
    gate_cut = jnp.minimum(gate_pre, clamp_limit)
    up_cut = jnp.clip(up_pre, -clamp_limit, clamp_limit)
    return ((up_cut + 1.0) * gate_cut * jax.nn.sigmoid(sigmoid_slope * gate_cut)).astype(jnp.bfloat16)

def reference(queries, keys, values, query_gain, key_gain, out_weight, mixer_gain, expert_in, routes, route_weights, expert_gain, gate_w, up_w, down_w, ffn_out_gain):
    group_size = HEADS // KV_HEADS
    position = jnp.arange(LEN, dtype=jnp.int32)
    query_norm = grid_rotate(rms_scale(queries.astype(jnp.float32).reshape(LEN, HEADS, HEAD), query_gain), position).astype(jnp.bfloat16)
    key_norm = grid_rotate(rms_scale(keys.astype(jnp.float32).reshape(LEN, KV_HEADS, HEAD), key_gain), position).astype(jnp.bfloat16)
    key_wide = key_norm.astype(jnp.float32)
    value_wide = values.reshape(LEN, KV_HEADS, HEAD).astype(jnp.float32)
    score_scale = HEAD ** (-0.5)
    query_blocks = query_norm.reshape(LEN // GRID_W, GRID_W, KV_HEADS, group_size, HEAD)

    def attend_block(block_in):
        scores = jnp.einsum('qhgd,khd->hgqk', block_in.astype(jnp.float32), key_wide) * score_scale
        expo = jnp.exp(scores - lax.optimization_barrier(jnp.max(scores, axis=-1, keepdims=True)))
        total = lax.optimization_barrier(jnp.sum(expo, axis=-1))
        probs = lax.optimization_barrier(expo.astype(jnp.bfloat16))
        summed = jnp.einsum('hgqk,khd->qhgd', probs.astype(jnp.float32), value_wide)
        return (summed / jnp.transpose(total, (2, 0, 1))[..., None]).astype(jnp.bfloat16)
    attended = lax.map(attend_block, query_blocks).reshape(LEN, HEADS * HEAD)
    column_span = HEADS * HEAD // N_TP
    projected = jnp.zeros((LEN, D), jnp.float32)
    for member in range(N_TP):
        partial_term = jnp.dot(attended[:, member * column_span:(member + 1) * column_span], out_weight[member * column_span:(member + 1) * column_span], preferred_element_type=jnp.float32).astype(jnp.bfloat16)
        projected = projected + lax.optimization_barrier(partial_term).astype(jnp.float32)
    mixer_out = rms_scale(projected, mixer_gain).astype(jnp.bfloat16)
    normed = rms_scale(expert_in.astype(jnp.float32), expert_gain).astype(jnp.bfloat16)
    padded = jnp.concatenate([normed, jnp.zeros((1, D), jnp.bfloat16)], axis=0)
    pair_expert = routes.reshape(-1)
    pair_count = pair_expert.shape[0]
    pair_weight = jnp.concatenate([route_weights.reshape(-1), jnp.zeros((1,), jnp.float32)], axis=0)
    most_rows = N_EP * N_TP * CAP
    hidden_span = FF // N_TP

    def one_expert(combined_in, expert_id):
        chosen = jnp.nonzero(pair_expert == expert_id, size=most_rows, fill_value=pair_count)[0].astype(jnp.int32)
        token_index = chosen // TOPK
        inputs = padded[token_index]
        hidden = clamped_unit(jnp.dot(inputs, gate_w[expert_id], preferred_element_type=jnp.float32), jnp.dot(inputs, up_w[expert_id], preferred_element_type=jnp.float32))
        down_here = down_w[expert_id]
        result = jnp.zeros((most_rows, D), jnp.float32)
        for member in range(N_TP):
            partial_term = jnp.dot(hidden[:, member * hidden_span:(member + 1) * hidden_span], down_here[member * hidden_span:(member + 1) * hidden_span], preferred_element_type=jnp.float32).astype(jnp.bfloat16)
            result = result + lax.optimization_barrier(partial_term).astype(jnp.float32)
        output_rows = lax.optimization_barrier(result.astype(jnp.bfloat16))
        combined_out = combined_in.at[token_index].add(pair_weight[chosen][:, None] * output_rows.astype(jnp.float32))
        return (combined_out, None)
    combined, unused = lax.scan(one_expert, jnp.zeros((TOKB + 1, D), jnp.float32), jnp.arange(EXPERTS, dtype=jnp.int32))
    expert_out = rms_scale(combined[:TOKB], ffn_out_gain).astype(jnp.bfloat16)
    return (mixer_out, expert_out)
```

```python
import jax
import jax.numpy as jnp
from jax import lax
from jax.experimental import pallas as pl
from jax.experimental.pallas import tpu as pltpu
from jax.sharding import PartitionSpec as P

HEAD = 128
GRID_W = 64


norm_eps = 1e-06
rope_base = 10000.0
clamp_limit = 7.0
sigmoid_slope = 1.702


def rms_scale(values_in, gain):
    return (
        values_in
        * lax.rsqrt(jnp.mean(values_in * values_in, axis=-1, keepdims=True) + norm_eps)
        * gain
    )


def turn_pair(halfpart, cosine, sine):
    first_part, second_part = jnp.split(halfpart, 2, axis=-1)
    return jnp.concatenate(
        [first_part * cosine - second_part * sine, second_part * cosine + first_part * sine],
        axis=-1,
    )


def grid_rotate(field, position):
    half_width = field.shape[-1] // 2
    inverse = rope_base ** (-jnp.arange(0, half_width, 2, dtype=jnp.float32) / half_width)
    grid_row = (position // GRID_W).astype(jnp.float32)
    grid_col = (position % GRID_W).astype(jnp.float32)
    row_angle = (grid_row[:, None] * inverse[None, :])[:, None, :]
    col_angle = (grid_col[:, None] * inverse[None, :])[:, None, :]
    return jnp.concatenate(
        [
            turn_pair(field[..., :half_width], jnp.cos(row_angle), jnp.sin(row_angle)),
            turn_pair(field[..., half_width:], jnp.cos(col_angle), jnp.sin(col_angle)),
        ],
        axis=-1,
    )


def clamped_unit(gate_pre, up_pre):
    gate_cut = jnp.minimum(gate_pre, clamp_limit)
    up_cut = jnp.clip(up_pre, -clamp_limit, clamp_limit)
    return ((up_cut + 1.0) * gate_cut * jax.nn.sigmoid(sigmoid_slope * gate_cut)).astype(
        jnp.bfloat16
    )


def mixer_half(queries, keys, values, query_gain, key_gain, out_weight, mixer_gain):
    local_rows = queries.shape[0]
    kv_local = keys.shape[1] // HEAD
    group_size = queries.shape[1] // HEAD // kv_local
    position = lax.axis_index("ep") * local_rows + jnp.arange(local_rows, dtype=jnp.int32)
    query_f = queries.astype(jnp.float32).reshape(local_rows, kv_local * group_size, HEAD)
    query_norm = grid_rotate(rms_scale(query_f, query_gain), position).astype(jnp.bfloat16)
    query_norm = query_norm.reshape(local_rows, kv_local, group_size, HEAD)
    key_f = keys.astype(jnp.float32).reshape(local_rows, kv_local, HEAD)
    key_norm = grid_rotate(rms_scale(key_f, key_gain), position).astype(jnp.bfloat16)
    key_norm = key_norm.reshape(local_rows, kv_local * HEAD)
    score_scale = HEAD ** (-0.5)
    initial = (
        jnp.full((kv_local, group_size, local_rows), -1e30, jnp.float32),
        jnp.zeros((kv_local, group_size, local_rows), jnp.float32),
        jnp.zeros((kv_local, group_size, local_rows, HEAD), jnp.float32),
    )
    key_piece = lax.all_gather(key_norm, "ep", axis=0, tiled=True)
    value_piece = lax.all_gather(values, "ep", axis=0, tiled=True)
    piece_rows = key_piece.shape[0]
    block_rows = 1
    for candidate in range(min(piece_rows, 1024), 0, -1):
        if piece_rows % candidate == 0:
            block_rows = candidate
            break
    key_blocks = key_piece.reshape(piece_rows // block_rows, block_rows, kv_local, HEAD)
    value_blocks = value_piece.reshape(piece_rows // block_rows, block_rows, kv_local, HEAD)

    def one_block(state, blocks_in):
        running_max, running_total, weighted = state
        key_block, value_block = blocks_in
        scores = (
            jnp.einsum("qhgd,khd->hgqk", query_norm, key_block, preferred_element_type=jnp.float32)
            * score_scale
        )
        new_max = jnp.maximum(running_max, jnp.max(scores, axis=-1))
        factor = jnp.exp(running_max - new_max)
        expo = jnp.exp(scores - new_max[..., None])
        new_total = running_total * factor + jnp.sum(expo, axis=-1)
        new_weighted = weighted * factor[..., None] + jnp.einsum(
            "hgqk,khd->hgqd",
            expo.astype(jnp.bfloat16),
            value_block,
            preferred_element_type=jnp.float32,
        )
        return ((new_max, new_total, new_weighted), None)

    state_out, unused = lax.scan(one_block, initial, (key_blocks, value_blocks))
    final_max, final_total, weighted = state_out
    attended = (weighted / final_total[..., None]).astype(jnp.bfloat16)
    attended = jnp.transpose(attended, (2, 0, 1, 3)).reshape(
        local_rows, kv_local * group_size * HEAD
    )
    share_rows = local_rows // lax.axis_size("tp")
    selected = lax.slice_in_dim(attended, 0, lax.axis_size("tp") * share_rows, axis=0)
    projected = lax.psum_scatter(
        jnp.dot(selected, out_weight, preferred_element_type=jnp.float32).astype(jnp.bfloat16),
        "tp",
        scatter_dimension=0,
        tiled=True,
    ).astype(jnp.float32)
    return rms_scale(projected, mixer_gain).astype(jnp.bfloat16)


def expert_half(expert_in, routes, route_weights, expert_gain, gate_w, up_w, down_w, ffn_out_gain):
    tok_rows = expert_in.shape[0]
    model_width = expert_in.shape[1]
    top_count = routes.shape[1]
    expert_count = lax.axis_size("ep")
    capacity = max(2, (3 * tok_rows * top_count + 2 * expert_count - 1) // (2 * expert_count))
    normed = rms_scale(expert_in.astype(jnp.float32), expert_gain).astype(jnp.bfloat16)
    pair_expert = routes.reshape(-1)
    pair_count = pair_expert.shape[0]
    one_hot = (pair_expert[:, None] == jnp.arange(expert_count, dtype=jnp.int32)[None, :]).astype(
        jnp.int32
    )
    pair_rank = jnp.sum(jnp.cumsum(one_hot, axis=0) * one_hot, axis=1) - 1
    pair_slot = pair_expert * capacity + pair_rank
    slot_pair = (
        jnp.full((expert_count * capacity,), pair_count, jnp.int32)
        .at[pair_slot]
        .set(jnp.arange(pair_count, dtype=jnp.int32))
    )
    padded = jnp.concatenate([normed, jnp.zeros((1, model_width), jnp.bfloat16)], axis=0)
    outgoing = padded[slot_pair // top_count].reshape(expert_count, capacity, model_width)
    gate_local = gate_w[0]
    up_local = up_w[0]
    down_local = down_w[0]
    arrived = lax.all_to_all(outgoing, "ep", split_axis=0, concat_axis=0, tiled=True)
    flat_rows = arrived.reshape(-1, model_width)
    shard_rows = lax.all_gather(flat_rows, "tp", axis=0, tiled=True)
    hidden = clamped_unit(
        jnp.dot(shard_rows, gate_local, preferred_element_type=jnp.float32),
        jnp.dot(shard_rows, up_local, preferred_element_type=jnp.float32),
    )
    selected = lax.slice_in_dim(hidden, 0, lax.axis_size("tp") * flat_rows.shape[0], axis=0)
    result = lax.psum_scatter(
        jnp.dot(selected, down_local, preferred_element_type=jnp.float32).astype(jnp.bfloat16),
        "tp",
        scatter_dimension=0,
        tiled=True,
    )
    finished = result.reshape(arrived.shape)
    returned = lax.all_to_all(finished, "ep", split_axis=0, concat_axis=0, tiled=True)
    pair_result = returned.reshape(-1, model_width)[pair_slot].reshape(
        tok_rows, top_count, model_width
    )
    combined = jnp.einsum("tk,tkd->td", route_weights, pair_result.astype(jnp.float32))
    return rms_scale(combined, ffn_out_gain).astype(jnp.bfloat16)


def flip(index, bits):
    power = 1
    while power <= bits:
        if bits & power:
            index = index + power - 2 * power * lax.rem(lax.div(index, power), 2)
        power *= 2
    return index


def peer_order(count):
    far = [j for j in range(count // 2, count) if j > 1]
    near = [j for j in range(2, count // 2)]
    order = [0, 1]
    while far or near:
        if far:
            order.append(far.pop(0))
        if near:
            order.append(near.pop(0))
    return order[:count]


def capacity_of(tok_rows, top_count, expert_count):
    return max(2, (3 * tok_rows * top_count + 2 * expert_count - 1) // (2 * expert_count))


def fused_fits(queries, keys, expert_in, routes, gate_w):
    n_ep, n_tp = lax.axis_size("ep"), lax.axis_size("tp")
    rows = queries.shape[0]
    capacity = capacity_of(expert_in.shape[0], routes.shape[1], n_ep)
    width = expert_in.shape[1]
    hidden = gate_w.shape[2]
    slots = n_ep * capacity
    held = 2 * width * slots * 14 + 6 * width * hidden * 4 + 4 * rows * rows * n_ep
    return (
        n_tp == 4
        and n_ep >= 4
        and n_ep & (n_ep - 1) == 0
        and keys.shape[1] == HEAD
        and capacity % 16 == 0
        and rows % (16 * n_tp) == 0
        and expert_in.shape[0] % 16 == 0
        and held < 56 * 2**20
    )


def fused_kernel(
    order,
    out_ref_q,
    kv_ref,
    outg_ref,
    weight_ref,
    mixer_gain_ref,
    ffn_gain_ref,
    out_w_hbm,
    gate_hbm,
    up_hbm,
    down_hbm,
    mixer_out_ref,
    expert_out_ref,
    out_w,
    gate,
    up,
    down,
    kv_all,
    att,
    proj,
    proj_in,
    proj_sum,
    proj_xin,
    rows,
    part,
    part_in,
    part_sum,
    part_xin,
    final,
    ret,
    w_sem,
    own_sem,
    kv_send,
    kv_recv,
    disp_send,
    disp_recv,
    core_send,
    core_recv,
    chip_send,
    chip_recv,
    relay_send,
    relay_recv,
    pcore_send,
    pcore_recv,
    pchip_send,
    pchip_recv,
    ret_send,
    ret_recv,
    mix_send,
    mix_recv,
):
    q_ref = out_ref_q
    n = len(order)
    width = rows.shape[1]
    cap = ret.shape[0] // n
    local_rows = kv_ref.shape[0]
    share = local_rows // 4
    heads = q_ref.shape[0] // local_rows
    ep, tp = lax.axis_index("ep"), lax.axis_index("tp")

    def at(ref, start, size):
        return ref.at[pl.ds(start, size), :]

    def remote(src, dst, send, recv, ep_bits, tp_bits):
        return pltpu.make_async_remote_copy(
            src_ref=src,
            dst_ref=dst,
            send_sem=send,
            recv_sem=recv,
            device_id={"ep": flip(ep, ep_bits), "tp": flip(tp, tp_bits)},
            device_id_type=pl.DeviceIdType.MESH,
        )

    loads = [
        pltpu.make_async_copy(a, b, w_sem.at[i])
        for i, (a, b) in enumerate(
            [(gate_hbm, gate), (up_hbm, up), (down_hbm, down), (out_w_hbm, out_w)]
        )
    ]
    for load in loads:
        load.start()
    own_kv = pltpu.make_async_copy(kv_ref, at(kv_all, 0, local_rows), own_sem.at[0])
    own_rows = pltpu.make_async_copy(at(outg_ref, 0, cap), at(rows, 0, cap), own_sem.at[1])
    own_kv.start()
    own_rows.start()

    barrier = pltpu.get_barrier_semaphore()
    peers = [(j, 0) for j in range(1, n)] + [(0, 1), (0, 2)]
    for ep_bits, tp_bits in peers:
        pl.semaphore_signal(
            barrier,
            inc=1,
            device_id={"ep": flip(ep, ep_bits), "tp": flip(tp, tp_bits)},
            device_id_type=pl.DeviceIdType.MESH,
        )
    pl.semaphore_wait(barrier, len(peers))

    kv_stages = []
    held = [0]
    bit = n // 2
    while bit >= 1:
        stage = []
        for block in held:
            source = kv_ref if block == 0 else at(kv_all, block * local_rows, local_rows)
            slot = block + bit
            stage.append(
                remote(
                    source,
                    at(kv_all, slot * local_rows, local_rows),
                    kv_send.at[slot],
                    kv_recv.at[slot],
                    bit,
                    0,
                )
            )
        kv_stages.append(stage)
        held = held + [block + bit for block in held]
        bit //= 2

    def place(slot, which):
        return (4 * slot + which) * cap

    dispatch = [
        None
        if j == 0
        else remote(
            at(outg_ref, k * cap, cap),
            at(rows, place(k, 0), cap),
            disp_send.at[k],
            disp_recv.at[k],
            j,
            0,
        )
        for k, j in enumerate(order)
    ]
    to_core, to_chip, relay = [], [], []
    p_core, p_chip, give_back = [], [], []
    for k, j in enumerate(order):
        source = at(outg_ref, 0, cap) if j == 0 else at(rows, place(k, 0), cap)
        to_core.append(
            remote(source, at(rows, place(k, 2), cap), core_send.at[k], core_recv.at[k], 0, 1)
        )
        to_chip.append(
            remote(source, at(rows, place(k, 1), cap), chip_send.at[k], chip_recv.at[k], 0, 2)
        )
        relay.append(
            remote(
                at(rows, place(k, 1), cap),
                at(rows, place(k, 3), cap),
                relay_send.at[k],
                relay_recv.at[k],
                0,
                1,
            )
        )
        p_core.append(
            remote(
                at(part, place(k, 2), 2 * cap),
                at(part_in, 2 * k * cap, 2 * cap),
                pcore_send.at[k],
                pcore_recv.at[k],
                0,
                1,
            )
        )
        p_chip.append(
            remote(
                at(part_sum, k * cap, cap),
                at(part_xin, k * cap, cap),
                pchip_send.at[k],
                pchip_recv.at[k],
                0,
                2,
            )
        )
        give_back.append(
            None
            if j == 0
            else remote(
                at(final, k * cap, cap),
                at(ret, k * cap, cap),
                ret_send.at[k],
                ret_recv.at[k],
                j,
                0,
            )
        )

    def pair(group):
        return (2 * group, 2 * group + 1)

    def forward(group):
        for k in pair(group):
            if dispatch[k] is not None:
                dispatch[k].wait_recv()
            to_chip[k].start()
            to_core[k].start()

    def pass_on(group):
        for k in pair(group):
            to_chip[k].wait_recv()
            relay[k].start()

    def compute(group):
        for k in pair(group):
            to_core[k].wait_recv()
            relay[k].wait_recv()
        span = pl.ds(place(2 * group, 0), 8 * cap)
        taken = rows[span, :]
        hidden = clamped_unit(
            jnp.dot(taken, gate[...], preferred_element_type=jnp.float32),
            jnp.dot(taken, up[...], preferred_element_type=jnp.float32),
        )
        part[span, :] = jnp.dot(hidden, down[...], preferred_element_type=jnp.float32).astype(
            jnp.bfloat16
        )
        for k in pair(group):
            p_core[k].start()

    def wide(ref, start, size):
        return ref[pl.ds(start, size), :].astype(jnp.float32)

    def reduce_core(group):
        for k in pair(group):
            p_core[k].wait_recv()
            part_sum[pl.ds(k * cap, cap), :] = (
                wide(part, place(k, 1), cap) + wide(part_in, (2 * k + 1) * cap, cap)
            ).astype(jnp.bfloat16)
            p_chip[k].start()

    def reduce_chip(group):
        for k in pair(group):
            p_chip[k].wait_recv()
            summed = (
                wide(part, place(k, 0), cap)
                + wide(part_in, 2 * k * cap, cap)
                + wide(part_xin, k * cap, cap)
            ).astype(jnp.bfloat16)
            if give_back[k] is None:
                ret[pl.ds(k * cap, cap), :] = summed
            else:
                final[pl.ds(k * cap, cap), :] = summed
                give_back[k].start()

    def attend(head):
        query = q_ref[pl.ds(head * local_rows, local_rows), :]
        scores = lax.dot_general(
            query,
            kv_all[:, :HEAD],
            (((1,), (1,)), ((), ())),
            preferred_element_type=jnp.float32,
        ) * (HEAD ** (-0.5))
        expo = jnp.exp(scores - jnp.max(scores, axis=-1, keepdims=True))
        total = jnp.sum(expo, axis=-1, keepdims=True)
        summed = jnp.dot(
            expo.astype(jnp.bfloat16), kv_all[:, HEAD:], preferred_element_type=jnp.float32
        )
        att[:, head * HEAD : (head + 1) * HEAD] = (summed / total).astype(jnp.bfloat16)

    def block_of(bits):
        return pl.multiple_of(flip(tp, bits) * share, share)

    mix_core = [
        remote(
            at(proj, block_of(1), share),
            at(proj_in, 0, share),
            mix_send.at[0],
            mix_recv.at[0],
            0,
            1,
        ),
        remote(
            at(proj, block_of(3), share),
            at(proj_in, share, share),
            mix_send.at[1],
            mix_recv.at[1],
            0,
            1,
        ),
    ]
    mix_chip = remote(proj_sum, proj_xin, mix_send.at[2], mix_recv.at[2], 0, 2)

    def project():
        proj[...] = jnp.dot(att[...], out_w[...], preferred_element_type=jnp.float32).astype(
            jnp.bfloat16
        )
        for copy in mix_core:
            copy.start()

    def mix_reduce():
        for copy in mix_core:
            copy.wait_recv()
        proj_sum[...] = (wide(proj, block_of(2), share) + wide(proj_in, share, share)).astype(
            jnp.bfloat16
        )
        mix_chip.start()

    def mix_finish():
        mix_chip.wait_recv()
        summed = (
            wide(proj, block_of(0), share)
            + wide(proj_in, 0, share)
            + proj_xin[...].astype(jnp.float32)
        )
        mixer_out_ref[...] = rms_scale(summed, mixer_gain_ref[...]).astype(jnp.bfloat16)

    kv_stages[0][0].start()
    for copy in dispatch:
        if copy is not None:
            copy.start()
    for copies, later in zip(kv_stages[:-1], kv_stages[1:]):
        if copies is kv_stages[0]:
            own_rows.wait()
        for copy in copies:
            copy.wait_recv()
        for copy in later:
            copy.start()
    forward(0)
    pass_on(0)
    loads[0].wait()
    loads[1].wait()
    loads[2].wait()
    groups = n // 2
    compute(0)
    forward(1)
    own_kv.wait()
    for copy in kv_stages[-1]:
        copy.wait_recv()
    for head in range(heads):
        attend(head)
        if head == heads // 2 - 1:
            pass_on(1)
            reduce_core(0)
    loads[3].wait()
    project()
    reduce_chip(0)
    for group in range(1, groups):
        if group + 1 < groups:
            forward(group + 1)
        compute(group)
        if group == 1:
            mix_reduce()
        if group + 1 < groups:
            pass_on(group + 1)
        if group >= 2:
            reduce_chip(group - 1)
        reduce_core(group)
    mix_finish()
    reduce_chip(groups - 1)
    for copy in give_back:
        if copy is not None:
            copy.wait_recv()

    rest = weight_ref[...]
    combined = jnp.zeros((weight_ref.shape[0], width), jnp.float32)
    for _ in range(3):
        piece = rest.astype(jnp.bfloat16)
        rest = rest - piece.astype(jnp.float32)
        combined = combined + jnp.dot(piece, ret[...], preferred_element_type=jnp.float32)
    expert_out_ref[...] = rms_scale(combined, ffn_gain_ref[...]).astype(jnp.bfloat16)

    for copy in (
        [c for stage in kv_stages for c in stage]
        + dispatch
        + to_core
        + to_chip
        + relay
        + p_core
        + p_chip
        + give_back
        + mix_core
        + [mix_chip]
    ):
        if copy is not None:
            copy.wait_send()


def fused_local(
    queries,
    keys,
    values,
    query_gain,
    key_gain,
    out_weight,
    mixer_gain,
    expert_in,
    routes,
    route_weights,
    expert_gain,
    gate_w,
    up_w,
    down_w,
    ffn_out_gain,
):
    n = lax.axis_size("ep")
    order = peer_order(n)
    local_rows = queries.shape[0]
    heads = queries.shape[1] // HEAD
    tok_rows, width = expert_in.shape
    cap = capacity_of(tok_rows, routes.shape[1], n)
    hidden = gate_w.shape[2]
    share = local_rows // 4
    ep = lax.axis_index("ep")

    position = ep * local_rows + jnp.arange(local_rows, dtype=jnp.int32)
    both = jnp.concatenate([queries, keys], axis=1).astype(jnp.float32)
    both = both.reshape(local_rows, heads + 1, HEAD)
    gains = jnp.concatenate(
        [jnp.broadcast_to(query_gain, (heads, HEAD)), key_gain[None]], axis=0
    )
    turned = grid_rotate(rms_scale(both, gains), position).astype(jnp.bfloat16)
    query_norm = jnp.transpose(turned[:, :heads], (1, 0, 2)).reshape(heads * local_rows, HEAD)
    key_value = jnp.concatenate([turned[:, heads], values], axis=1)

    normed = rms_scale(expert_in.astype(jnp.float32), expert_gain).astype(jnp.bfloat16)
    slot_expert = jnp.bitwise_xor(ep.astype(jnp.int32), jnp.array(order, jnp.int32))
    named = routes[:, :, None] == slot_expert[None, None, :]
    chosen = jnp.any(named, axis=1)
    weight = jnp.sum(jnp.where(named, route_weights[:, :, None], 0.0), axis=1)
    token = jnp.arange(tok_rows, dtype=jnp.int32)
    earlier = (token[:, None] > token[None, :]).astype(jnp.bfloat16)
    rank = jnp.dot(earlier, chosen.astype(jnp.bfloat16), preferred_element_type=jnp.float32)
    rank = rank.astype(jnp.int32)
    taken = chosen[:, :, None] & (rank[:, :, None] == jnp.arange(cap, dtype=jnp.int32))
    slot_weight = jnp.where(taken, weight[:, :, None], 0.0).reshape(tok_rows, n * cap)
    pick = taken.astype(jnp.bfloat16).reshape(tok_rows, n * cap)
    outgoing = lax.dot_general(
        pick, normed, (((0,), (0,)), ((), ())), preferred_element_type=jnp.float32
    ).astype(jnp.bfloat16)

    vmem = pl.BlockSpec(memory_space=pltpu.VMEM)
    anywhere = pl.BlockSpec(memory_space=pl.ANY)
    bf16 = jnp.bfloat16
    dma = pltpu.SemaphoreType.DMA

    def fused(*refs):
        return fused_kernel(order, *refs)

    return pl.pallas_call(
        fused,
        out_shape=(
            jax.ShapeDtypeStruct((share, width), bf16),
            jax.ShapeDtypeStruct((tok_rows, width), bf16),
        ),
        in_specs=[vmem] * 6 + [anywhere] * 4,
        out_specs=(vmem, vmem),
        scratch_shapes=[
            pltpu.VMEM((heads * HEAD, width), bf16),
            pltpu.VMEM((width, hidden), bf16),
            pltpu.VMEM((width, hidden), bf16),
            pltpu.VMEM((hidden, width), bf16),
            pltpu.VMEM((n * local_rows, 2 * HEAD), bf16),
            pltpu.VMEM((local_rows, heads * HEAD), bf16),
            pltpu.VMEM((local_rows, width), bf16),
            pltpu.VMEM((2 * share, width), bf16),
            pltpu.VMEM((share, width), bf16),
            pltpu.VMEM((share, width), bf16),
            pltpu.VMEM((4 * n * cap, width), bf16),
            pltpu.VMEM((4 * n * cap, width), bf16),
            pltpu.VMEM((2 * n * cap, width), bf16),
            pltpu.VMEM((n * cap, width), bf16),
            pltpu.VMEM((n * cap, width), bf16),
            pltpu.VMEM((n * cap, width), bf16),
            pltpu.VMEM((n * cap, width), bf16),
            dma((4,)),
            dma((2,)),
        ]
        + [dma((n,))] * 16
        + [dma((3,))] * 2,
        compiler_params=pltpu.CompilerParams(
            collective_id=0, has_side_effects=True, vmem_limit_bytes=60 * 2**20
        ),
    )(
        query_norm,
        key_value,
        outgoing,
        slot_weight,
        mixer_gain[None],
        ffn_out_gain[None],
        out_weight,
        gate_w[0],
        up_w[0],
        down_w[0],
    )


def local(
    queries,
    keys,
    values,
    query_gain,
    key_gain,
    out_weight,
    mixer_gain,
    expert_in,
    routes,
    route_weights,
    expert_gain,
    gate_w,
    up_w,
    down_w,
    ffn_out_gain,
):
    if fused_fits(queries, keys, expert_in, routes, gate_w):
        return fused_local(
            queries, keys, values, query_gain, key_gain, out_weight, mixer_gain, expert_in, routes,
            route_weights, expert_gain, gate_w, up_w, down_w, ffn_out_gain,
        )
    mixer_out = mixer_half(queries, keys, values, query_gain, key_gain, out_weight, mixer_gain)
    expert_out = expert_half(
        expert_in, routes, route_weights, expert_gain, gate_w, up_w, down_w, ffn_out_gain
    )
    return (mixer_out, expert_out)


def solution(mesh):
    in_specs = (
        P("ep", "tp"),
        P("ep", "tp"),
        P("ep", "tp"),
        P(),
        P(),
        P("tp", None),
        P(),
        P(("ep", "tp"), None),
        P(("ep", "tp"), None),
        P(("ep", "tp"), None),
        P(),
        P("ep", None, "tp"),
        P("ep", None, "tp"),
        P("ep", "tp", None),
        P(),
    )
    out_specs = (P(("ep", "tp"), None), P(("ep", "tp"), None))
    return jax.shard_map(local, mesh=mesh, in_specs=in_specs, out_specs=out_specs, check_vma=False)
```

```python
import jax
import jax.numpy as jnp
from jax import lax
from jax.experimental import pallas as pl
from jax.experimental.pallas import tpu as pltpu
from jax.sharding import PartitionSpec as P

HEAD = 128
GRID_W = 64


norm_eps = 1e-06
rope_base = 10000.0
clamp_limit = 7.0
sigmoid_slope = 1.702


def rms_scale(values_in, gain):
    return (
        values_in
        * lax.rsqrt(jnp.mean(values_in * values_in, axis=-1, keepdims=True) + norm_eps)
        * gain
    )


def turn_pair(halfpart, cosine, sine):
    first_part, second_part = jnp.split(halfpart, 2, axis=-1)
    return jnp.concatenate(
        [first_part * cosine - second_part * sine, second_part * cosine + first_part * sine],
        axis=-1,
    )


def grid_rotate(field, position):
    half_width = field.shape[-1] // 2
    inverse = rope_base ** (-jnp.arange(0, half_width, 2, dtype=jnp.float32) / half_width)
    grid_row = (position // GRID_W).astype(jnp.float32)
    grid_col = (position % GRID_W).astype(jnp.float32)
    row_angle = (grid_row[:, None] * inverse[None, :])[:, None, :]
    col_angle = (grid_col[:, None] * inverse[None, :])[:, None, :]
    return jnp.concatenate(
        [
            turn_pair(field[..., :half_width], jnp.cos(row_angle), jnp.sin(row_angle)),
            turn_pair(field[..., half_width:], jnp.cos(col_angle), jnp.sin(col_angle)),
        ],
        axis=-1,
    )


def clamped_unit(gate_pre, up_pre):
    gate_cut = jnp.minimum(gate_pre, clamp_limit)
    up_cut = jnp.clip(up_pre, -clamp_limit, clamp_limit)
    return ((up_cut + 1.0) * gate_cut * jax.nn.sigmoid(sigmoid_slope * gate_cut)).astype(
        jnp.bfloat16
    )


def mixer_half(queries, keys, values, query_gain, key_gain, out_weight, mixer_gain):
    local_rows = queries.shape[0]
    kv_local = keys.shape[1] // HEAD
    group_size = queries.shape[1] // HEAD // kv_local
    position = lax.axis_index("ep") * local_rows + jnp.arange(local_rows, dtype=jnp.int32)
    query_f = queries.astype(jnp.float32).reshape(local_rows, kv_local * group_size, HEAD)
    query_norm = grid_rotate(rms_scale(query_f, query_gain), position).astype(jnp.bfloat16)
    query_norm = query_norm.reshape(local_rows, kv_local, group_size, HEAD)
    key_f = keys.astype(jnp.float32).reshape(local_rows, kv_local, HEAD)
    key_norm = grid_rotate(rms_scale(key_f, key_gain), position).astype(jnp.bfloat16)
    key_norm = key_norm.reshape(local_rows, kv_local * HEAD)
    score_scale = HEAD ** (-0.5)
    initial = (
        jnp.full((kv_local, group_size, local_rows), -1e30, jnp.float32),
        jnp.zeros((kv_local, group_size, local_rows), jnp.float32),
        jnp.zeros((kv_local, group_size, local_rows, HEAD), jnp.float32),
    )
    key_piece = lax.all_gather(key_norm, "ep", axis=0, tiled=True)
    value_piece = lax.all_gather(values, "ep", axis=0, tiled=True)
    piece_rows = key_piece.shape[0]
    block_rows = 1
    for candidate in range(min(piece_rows, 1024), 0, -1):
        if piece_rows % candidate == 0:
            block_rows = candidate
            break
    key_blocks = key_piece.reshape(piece_rows // block_rows, block_rows, kv_local, HEAD)
    value_blocks = value_piece.reshape(piece_rows // block_rows, block_rows, kv_local, HEAD)

    def one_block(state, blocks_in):
        running_max, running_total, weighted = state
        key_block, value_block = blocks_in
        scores = (
            jnp.einsum("qhgd,khd->hgqk", query_norm, key_block, preferred_element_type=jnp.float32)
            * score_scale
        )
        new_max = jnp.maximum(running_max, jnp.max(scores, axis=-1))
        factor = jnp.exp(running_max - new_max)
        expo = jnp.exp(scores - new_max[..., None])
        new_total = running_total * factor + jnp.sum(expo, axis=-1)
        new_weighted = weighted * factor[..., None] + jnp.einsum(
            "hgqk,khd->hgqd",
            expo.astype(jnp.bfloat16),
            value_block,
            preferred_element_type=jnp.float32,
        )
        return ((new_max, new_total, new_weighted), None)

    state_out, unused = lax.scan(one_block, initial, (key_blocks, value_blocks))
    final_max, final_total, weighted = state_out
    attended = (weighted / final_total[..., None]).astype(jnp.bfloat16)
    attended = jnp.transpose(attended, (2, 0, 1, 3)).reshape(
        local_rows, kv_local * group_size * HEAD
    )
    share_rows = local_rows // lax.axis_size("tp")
    selected = lax.slice_in_dim(attended, 0, lax.axis_size("tp") * share_rows, axis=0)
    projected = lax.psum_scatter(
        jnp.dot(selected, out_weight, preferred_element_type=jnp.float32).astype(jnp.bfloat16),
        "tp",
        scatter_dimension=0,
        tiled=True,
    ).astype(jnp.float32)
    return rms_scale(projected, mixer_gain).astype(jnp.bfloat16)


def expert_half(expert_in, routes, route_weights, expert_gain, gate_w, up_w, down_w, ffn_out_gain):
    tok_rows = expert_in.shape[0]
    model_width = expert_in.shape[1]
    top_count = routes.shape[1]
    expert_count = lax.axis_size("ep")
    capacity = max(2, (3 * tok_rows * top_count + 2 * expert_count - 1) // (2 * expert_count))
    normed = rms_scale(expert_in.astype(jnp.float32), expert_gain).astype(jnp.bfloat16)
    pair_expert = routes.reshape(-1)
    pair_count = pair_expert.shape[0]
    one_hot = (pair_expert[:, None] == jnp.arange(expert_count, dtype=jnp.int32)[None, :]).astype(
        jnp.int32
    )
    pair_rank = jnp.sum(jnp.cumsum(one_hot, axis=0) * one_hot, axis=1) - 1
    pair_slot = pair_expert * capacity + pair_rank
    slot_pair = (
        jnp.full((expert_count * capacity,), pair_count, jnp.int32)
        .at[pair_slot]
        .set(jnp.arange(pair_count, dtype=jnp.int32))
    )
    padded = jnp.concatenate([normed, jnp.zeros((1, model_width), jnp.bfloat16)], axis=0)
    outgoing = padded[slot_pair // top_count].reshape(expert_count, capacity, model_width)
    gate_local = gate_w[0]
    up_local = up_w[0]
    down_local = down_w[0]
    arrived = lax.all_to_all(outgoing, "ep", split_axis=0, concat_axis=0, tiled=True)
    flat_rows = arrived.reshape(-1, model_width)
    shard_rows = lax.all_gather(flat_rows, "tp", axis=0, tiled=True)
    hidden = clamped_unit(
        jnp.dot(shard_rows, gate_local, preferred_element_type=jnp.float32),
        jnp.dot(shard_rows, up_local, preferred_element_type=jnp.float32),
    )
    selected = lax.slice_in_dim(hidden, 0, lax.axis_size("tp") * flat_rows.shape[0], axis=0)
    result = lax.psum_scatter(
        jnp.dot(selected, down_local, preferred_element_type=jnp.float32).astype(jnp.bfloat16),
        "tp",
        scatter_dimension=0,
        tiled=True,
    )
    finished = result.reshape(arrived.shape)
    returned = lax.all_to_all(finished, "ep", split_axis=0, concat_axis=0, tiled=True)
    pair_result = returned.reshape(-1, model_width)[pair_slot].reshape(
        tok_rows, top_count, model_width
    )
    combined = jnp.einsum("tk,tkd->td", route_weights, pair_result.astype(jnp.float32))
    return rms_scale(combined, ffn_out_gain).astype(jnp.bfloat16)


def flip(index, bits):
    power = 1
    while power <= bits:
        if bits & power:
            index = index + power - 2 * power * lax.rem(lax.div(index, power), 2)
        power *= 2
    return index


def peer_order(count):
    far = [j for j in range(count // 2, count) if j > 1]
    near = [j for j in range(2, count // 2)]
    order = [0, 1]
    while far or near:
        if far:
            order.append(far.pop(0))
        if near:
            order.append(near.pop(0))
    return order[:count]


def capacity_of(tok_rows, top_count, expert_count):
    return max(2, (3 * tok_rows * top_count + 2 * expert_count - 1) // (2 * expert_count))


def fused_fits(queries, keys, expert_in, routes, gate_w):
    n_ep, n_tp = lax.axis_size("ep"), lax.axis_size("tp")
    rows = queries.shape[0]
    capacity = capacity_of(expert_in.shape[0], routes.shape[1], n_ep)
    width = expert_in.shape[1]
    hidden = gate_w.shape[2]
    slots = n_ep * capacity
    held = 2 * width * slots * 14 + 6 * width * hidden * 4 + 4 * rows * rows * n_ep
    return (
        n_tp == 4
        and n_ep >= 4
        and n_ep & (n_ep - 1) == 0
        and keys.shape[1] == HEAD
        and capacity % 16 == 0
        and rows % (16 * n_tp) == 0
        and expert_in.shape[0] % 16 == 0
        and held < 56 * 2**20
    )


def fused_kernel(
    order,
    out_ref_q,
    kv_ref,
    outg_ref,
    weight_ref,
    mixer_gain_ref,
    ffn_gain_ref,
    out_w_hbm,
    gate_hbm,
    up_hbm,
    down_hbm,
    mixer_out_ref,
    expert_out_ref,
    out_w,
    gate,
    up,
    down,
    kv_all,
    att,
    proj,
    proj_in,
    proj_sum,
    proj_xin,
    rows,
    part,
    part_in,
    part_sum,
    part_xin,
    final,
    ret,
    w_sem,
    own_sem,
    kv_send,
    kv_recv,
    disp_send,
    disp_recv,
    core_send,
    core_recv,
    chip_send,
    chip_recv,
    relay_send,
    relay_recv,
    pcore_send,
    pcore_recv,
    pchip_send,
    pchip_recv,
    ret_send,
    ret_recv,
    mix_send,
    mix_recv,
):
    q_ref = out_ref_q
    n = len(order)
    width = rows.shape[1]
    cap = ret.shape[0] // n
    local_rows = kv_ref.shape[0]
    share = local_rows // 4
    heads = q_ref.shape[0] // local_rows
    ep, tp = lax.axis_index("ep"), lax.axis_index("tp")

    def at(ref, start, size):
        return ref.at[pl.ds(start, size), :]

    def remote(src, dst, send, recv, ep_bits, tp_bits):
        return pltpu.make_async_remote_copy(
            src_ref=src,
            dst_ref=dst,
            send_sem=send,
            recv_sem=recv,
            device_id={"ep": flip(ep, ep_bits), "tp": flip(tp, tp_bits)},
            device_id_type=pl.DeviceIdType.MESH,
        )

    loads = [
        pltpu.make_async_copy(a, b, w_sem.at[i])
        for i, (a, b) in enumerate(
            [(gate_hbm, gate), (up_hbm, up), (down_hbm, down), (out_w_hbm, out_w)]
        )
    ]
    for load in loads:
        load.start()
    own_kv = pltpu.make_async_copy(kv_ref, at(kv_all, 0, local_rows), own_sem.at[0])
    own_rows = pltpu.make_async_copy(at(outg_ref, 0, cap), at(rows, 0, cap), own_sem.at[1])
    own_kv.start()
    own_rows.start()

    barrier = pltpu.get_barrier_semaphore()
    peers = [(j, 0) for j in range(1, n)] + [(0, 1), (0, 2)]
    for ep_bits, tp_bits in peers:
        pl.semaphore_signal(
            barrier,
            inc=1,
            device_id={"ep": flip(ep, ep_bits), "tp": flip(tp, tp_bits)},
            device_id_type=pl.DeviceIdType.MESH,
        )
    pl.semaphore_wait(barrier, len(peers))

    kv_stages = []
    held = [0]
    bit = n // 2
    while bit >= 1:
        stage = []
        for block in held:
            source = kv_ref if block == 0 else at(kv_all, block * local_rows, local_rows)
            slot = block + bit
            stage.append(
                remote(
                    source,
                    at(kv_all, slot * local_rows, local_rows),
                    kv_send.at[slot],
                    kv_recv.at[slot],
                    bit,
                    0,
                )
            )
        kv_stages.append(stage)
        held = held + [block + bit for block in held]
        bit //= 2

    def place(slot, which):
        return (4 * slot + which) * cap

    dispatch = [
        None
        if j == 0
        else remote(
            at(outg_ref, k * cap, cap),
            at(rows, place(k, 0), cap),
            disp_send.at[k],
            disp_recv.at[k],
            j,
            0,
        )
        for k, j in enumerate(order)
    ]
    to_core, to_chip, relay = [], [], []
    p_core, p_chip, give_back = [], [], []
    for k, j in enumerate(order):
        source = at(outg_ref, 0, cap) if j == 0 else at(rows, place(k, 0), cap)
        to_core.append(
            remote(source, at(rows, place(k, 2), cap), core_send.at[k], core_recv.at[k], 0, 1)
        )
        to_chip.append(
            remote(source, at(rows, place(k, 1), cap), chip_send.at[k], chip_recv.at[k], 0, 2)
        )
        relay.append(
            remote(
                at(rows, place(k, 1), cap),
                at(rows, place(k, 3), cap),
                relay_send.at[k],
                relay_recv.at[k],
                0,
                1,
            )
        )
        p_core.append(
            remote(
                at(part, place(k, 2), 2 * cap),
                at(part_in, 2 * k * cap, 2 * cap),
                pcore_send.at[k],
                pcore_recv.at[k],
                0,
                1,
            )
        )
        p_chip.append(
            remote(
                at(part_sum, k * cap, cap),
                at(part_xin, k * cap, cap),
                pchip_send.at[k],
                pchip_recv.at[k],
                0,
                2,
            )
        )
        give_back.append(
            None
            if j == 0
            else remote(
                at(final, k * cap, cap),
                at(ret, k * cap, cap),
                ret_send.at[k],
                ret_recv.at[k],
                j,
                0,
            )
        )

    def pair(group):
        return (2 * group, 2 * group + 1)

    def forward_one(k):
        if dispatch[k] is not None:
            dispatch[k].wait_recv()
        to_chip[k].start()
        to_core[k].start()

    def pass_on_one(k):
        to_chip[k].wait_recv()
        relay[k].start()

    def forward(group):
        for k in pair(group):
            forward_one(k)

    def pass_on(group):
        for k in pair(group):
            pass_on_one(k)

    def compute(group):
        for k in pair(group):
            to_core[k].wait_recv()
            relay[k].wait_recv()
        span = pl.ds(place(2 * group, 0), 8 * cap)
        taken = rows[span, :]
        hidden = clamped_unit(
            jnp.dot(taken, gate[...], preferred_element_type=jnp.float32),
            jnp.dot(taken, up[...], preferred_element_type=jnp.float32),
        )
        part[span, :] = jnp.dot(hidden, down[...], preferred_element_type=jnp.float32).astype(
            jnp.bfloat16
        )
        for k in pair(group):
            p_core[k].start()

    def wide(ref, start, size):
        return ref[pl.ds(start, size), :].astype(jnp.float32)

    def reduce_core(group):
        for k in pair(group):
            p_core[k].wait_recv()
            part_sum[pl.ds(k * cap, cap), :] = (
                wide(part, place(k, 1), cap) + wide(part_in, (2 * k + 1) * cap, cap)
            ).astype(jnp.bfloat16)
            p_chip[k].start()

    def reduce_chip(group):
        for k in pair(group):
            p_chip[k].wait_recv()
            summed = (
                wide(part, place(k, 0), cap)
                + wide(part_in, 2 * k * cap, cap)
                + wide(part_xin, k * cap, cap)
            ).astype(jnp.bfloat16)
            if give_back[k] is None:
                ret[pl.ds(k * cap, cap), :] = summed
            else:
                final[pl.ds(k * cap, cap), :] = summed
                give_back[k].start()

    def attend(head):
        query = q_ref[pl.ds(head * local_rows, local_rows), :]
        scores = lax.dot_general(
            query,
            kv_all[:, :HEAD],
            (((1,), (1,)), ((), ())),
            preferred_element_type=jnp.float32,
        ) * (HEAD ** (-0.5))
        expo = jnp.exp(scores - jnp.max(scores, axis=-1, keepdims=True))
        total = jnp.sum(expo, axis=-1, keepdims=True)
        summed = jnp.dot(
            expo.astype(jnp.bfloat16), kv_all[:, HEAD:], preferred_element_type=jnp.float32
        )
        att[:, head * HEAD : (head + 1) * HEAD] = (summed / total).astype(jnp.bfloat16)

    def block_of(bits):
        return pl.multiple_of(flip(tp, bits) * share, share)

    mix_core = [
        remote(
            at(proj, block_of(1), share),
            at(proj_in, 0, share),
            mix_send.at[0],
            mix_recv.at[0],
            0,
            1,
        ),
        remote(
            at(proj, block_of(3), share),
            at(proj_in, share, share),
            mix_send.at[1],
            mix_recv.at[1],
            0,
            1,
        ),
    ]
    mix_chip = remote(proj_sum, proj_xin, mix_send.at[2], mix_recv.at[2], 0, 2)

    def project():
        proj[...] = jnp.dot(att[...], out_w[...], preferred_element_type=jnp.float32).astype(
            jnp.bfloat16
        )
        for copy in mix_core:
            copy.start()

    def mix_reduce():
        for copy in mix_core:
            copy.wait_recv()
        proj_sum[...] = (wide(proj, block_of(2), share) + wide(proj_in, share, share)).astype(
            jnp.bfloat16
        )
        mix_chip.start()

    def mix_finish():
        mix_chip.wait_recv()
        summed = (
            wide(proj, block_of(0), share)
            + wide(proj_in, 0, share)
            + proj_xin[...].astype(jnp.float32)
        )
        mixer_out_ref[...] = rms_scale(summed, mixer_gain_ref[...]).astype(jnp.bfloat16)

    groups = n // 2
    for copy in kv_stages[0]:
        copy.start()
    dispatch[1].start()
    for k in range(2, 4):
        dispatch[k].start()
    forward_one(0)
    forward_one(1)
    for copies, later in zip(kv_stages[:-1], kv_stages[1:]):
        for copy in copies:
            copy.wait_recv()
        for copy in later:
            copy.start()
        if copies is kv_stages[0]:
            for k in range(4, n):
                dispatch[k].start()
            own_rows.wait()
            pass_on(0)
            for load in loads[:3]:
                load.wait()
            compute(0)
            forward(1)
            reduce_core(0)
    pass_on(1)
    own_kv.wait()
    for copy in kv_stages[-1]:
        copy.wait_recv()
    for group in range(1, groups):
        if group + 1 < groups:
            forward(group + 1)
        compute(group)
        if group < 2:
            reduce_chip(group - 1)
        if group + 1 < groups:
            pass_on(group + 1)
        if group == 1:
            for head in range(heads // 2):
                attend(head)
        reduce_core(group)
        if group >= 2:
            reduce_chip(group - 1)
        if group == 1:
            for head in range(heads // 2, heads):
                attend(head)
            loads[3].wait()
            project()
        if group == 2:
            mix_reduce()
    mix_finish()
    reduce_chip(groups - 1)
    for copy in give_back:
        if copy is not None:
            copy.wait_recv()

    rest = weight_ref[...]
    combined = jnp.zeros((weight_ref.shape[0], width), jnp.float32)
    for _ in range(3):
        piece = rest.astype(jnp.bfloat16)
        rest = rest - piece.astype(jnp.float32)
        combined = combined + jnp.dot(piece, ret[...], preferred_element_type=jnp.float32)
    expert_out_ref[...] = rms_scale(combined, ffn_gain_ref[...]).astype(jnp.bfloat16)

    for copy in (
        [c for stage in kv_stages for c in stage]
        + dispatch
        + to_core
        + to_chip
        + relay
        + p_core
        + p_chip
        + give_back
        + mix_core
        + [mix_chip]
    ):
        if copy is not None:
            copy.wait_send()


def fused_local(
    queries,
    keys,
    values,
    query_gain,
    key_gain,
    out_weight,
    mixer_gain,
    expert_in,
    routes,
    route_weights,
    expert_gain,
    gate_w,
    up_w,
    down_w,
    ffn_out_gain,
):
    n = lax.axis_size("ep")
    order = peer_order(n)
    local_rows = queries.shape[0]
    heads = queries.shape[1] // HEAD
    tok_rows, width = expert_in.shape
    cap = capacity_of(tok_rows, routes.shape[1], n)
    hidden = gate_w.shape[2]
    share = local_rows // 4
    ep = lax.axis_index("ep")

    position = ep * local_rows + jnp.arange(local_rows, dtype=jnp.int32)
    both = jnp.concatenate([queries, keys], axis=1).astype(jnp.float32)
    both = both.reshape(local_rows, heads + 1, HEAD)
    gains = jnp.concatenate(
        [jnp.broadcast_to(query_gain, (heads, HEAD)), key_gain[None]], axis=0
    )
    turned = grid_rotate(rms_scale(both, gains), position).astype(jnp.bfloat16)
    query_norm = jnp.transpose(turned[:, :heads], (1, 0, 2)).reshape(heads * local_rows, HEAD)
    key_value = jnp.concatenate([turned[:, heads], values], axis=1)

    normed = rms_scale(expert_in.astype(jnp.float32), expert_gain).astype(jnp.bfloat16)
    slot_expert = jnp.bitwise_xor(ep.astype(jnp.int32), jnp.array(order, jnp.int32))
    named = routes[:, :, None] == slot_expert[None, None, :]
    chosen = jnp.any(named, axis=1)
    weight = jnp.sum(jnp.where(named, route_weights[:, :, None], 0.0), axis=1)
    token = jnp.arange(tok_rows, dtype=jnp.int32)
    earlier = (token[:, None] > token[None, :]).astype(jnp.bfloat16)
    rank = jnp.dot(earlier, chosen.astype(jnp.bfloat16), preferred_element_type=jnp.float32)
    rank = rank.astype(jnp.int32)
    taken = chosen[:, :, None] & (rank[:, :, None] == jnp.arange(cap, dtype=jnp.int32))
    slot_weight = jnp.where(taken, weight[:, :, None], 0.0).reshape(tok_rows, n * cap)
    pick = taken.astype(jnp.bfloat16).reshape(tok_rows, n * cap)
    outgoing = lax.dot_general(
        pick, normed, (((0,), (0,)), ((), ())), preferred_element_type=jnp.float32
    ).astype(jnp.bfloat16)

    vmem = pl.BlockSpec(memory_space=pltpu.VMEM)
    anywhere = pl.BlockSpec(memory_space=pl.ANY)
    bf16 = jnp.bfloat16
    dma = pltpu.SemaphoreType.DMA

    def fused(*refs):
        return fused_kernel(order, *refs)

    return pl.pallas_call(
        fused,
        out_shape=(
            jax.ShapeDtypeStruct((share, width), bf16),
            jax.ShapeDtypeStruct((tok_rows, width), bf16),
        ),
        in_specs=[vmem] * 6 + [anywhere] * 4,
        out_specs=(vmem, vmem),
        scratch_shapes=[
            pltpu.VMEM((heads * HEAD, width), bf16),
            pltpu.VMEM((width, hidden), bf16),
            pltpu.VMEM((width, hidden), bf16),
            pltpu.VMEM((hidden, width), bf16),
            pltpu.VMEM((n * local_rows, 2 * HEAD), bf16),
            pltpu.VMEM((local_rows, heads * HEAD), bf16),
            pltpu.VMEM((local_rows, width), bf16),
            pltpu.VMEM((2 * share, width), bf16),
            pltpu.VMEM((share, width), bf16),
            pltpu.VMEM((share, width), bf16),
            pltpu.VMEM((4 * n * cap, width), bf16),
            pltpu.VMEM((4 * n * cap, width), bf16),
            pltpu.VMEM((2 * n * cap, width), bf16),
            pltpu.VMEM((n * cap, width), bf16),
            pltpu.VMEM((n * cap, width), bf16),
            pltpu.VMEM((n * cap, width), bf16),
            pltpu.VMEM((n * cap, width), bf16),
            dma((4,)),
            dma((2,)),
        ]
        + [dma((n,))] * 16
        + [dma((3,))] * 2,
        compiler_params=pltpu.CompilerParams(
            collective_id=0, has_side_effects=True, vmem_limit_bytes=60 * 2**20
        ),
    )(
        query_norm,
        key_value,
        outgoing,
        slot_weight,
        mixer_gain[None],
        ffn_out_gain[None],
        out_weight,
        gate_w[0],
        up_w[0],
        down_w[0],
    )


def local(
    queries,
    keys,
    values,
    query_gain,
    key_gain,
    out_weight,
    mixer_gain,
    expert_in,
    routes,
    route_weights,
    expert_gain,
    gate_w,
    up_w,
    down_w,
    ffn_out_gain,
):
    if fused_fits(queries, keys, expert_in, routes, gate_w):
        return fused_local(
            queries, keys, values, query_gain, key_gain, out_weight, mixer_gain, expert_in, routes,
            route_weights, expert_gain, gate_w, up_w, down_w, ffn_out_gain,
        )
    mixer_out = mixer_half(queries, keys, values, query_gain, key_gain, out_weight, mixer_gain)
    expert_out = expert_half(
        expert_in, routes, route_weights, expert_gain, gate_w, up_w, down_w, ffn_out_gain
    )
    return (mixer_out, expert_out)


def solution(mesh):
    in_specs = (
        P("ep", "tp"),
        P("ep", "tp"),
        P("ep", "tp"),
        P(),
        P(),
        P("tp", None),
        P(),
        P(("ep", "tp"), None),
        P(("ep", "tp"), None),
        P(("ep", "tp"), None),
        P(),
        P("ep", None, "tp"),
        P("ep", None, "tp"),
        P("ep", "tp", None),
        P(),
    )
    out_specs = (P(("ep", "tp"), None), P(("ep", "tp"), None))
    return jax.shard_map(local, mesh=mesh, in_specs=in_specs, out_specs=out_specs, check_vma=False)
```
